256 devices in a mesh: ep: 128 (over z, y, x), tp: 2 (over core).
Axes of the slice: x: 4, y: 4, z: 8, core: 2. Of those that a mesh axis runs over, the one named last changes fastest.
Arguments:
- tokens: bfloat16 [256, 2048], P('ep'), may hold values from -6 to 6
- head_state: float32 [256, 32, 64, 128], P('ep', 'tp'), may hold values from -4 to 4
- conv_state: bfloat16 [256, 3, 2048], P('ep', None, 'tp'), may hold values from -6 to 6
- conv_proj_state: bfloat16 [256, 3, 2, 512], P('ep', None, None, 'tp'), may hold values from -6 to 6
- first_gain: float32 [2048], replicated, may hold values from 0.1 to 1.9
- gate_weight: bfloat16 [2048, 2048], P('ep', 'tp'), may hold values from -0.125 to 0.125
- inner_weight: bfloat16 [2048, 2048], P('ep', 'tp'), may hold values from -0.125 to 0.125
- write_weight: bfloat16 [2048, 512], P(None, 'tp'), may hold values from -0.125 to 0.125
- read_weight: bfloat16 [2048, 512], P(None, 'tp'), may hold values from -0.125 to 0.125
- step_weight: bfloat16 [2048, 32], P(None, 'tp'), may hold values from -0.125 to 0.125
- conv_kernel: float32 [4, 2048], P(None, 'tp'), may hold values from -3 to 3
- conv_proj_kernel: float32 [4, 2, 512], P(None, None, 'tp'), may hold values from -3 to 3
- step_bias: float32 [32], P('tp'), may hold values from -2 to 1
- log_rate: float32 [32], P('tp'), may hold values from -4.5 to 1.5
- skip_gain: float32 [32], P('tp'), may hold values from 0.5 to 2
- group_gain: float32 [2048], P('tp'), may hold values from 0.1 to 1.9
- out_weight: bfloat16 [2048, 2048], P('tp', 'ep'), may hold values from -0.125 to 0.125
- second_gain: float32 [2048], replicated, may hold values from 0.1 to 1.9
- routes: int32 [256, 4], P('ep'), may hold values from 0 to 127, all different within a row; in each aligned block of 256 rows (0 to 255, 256 to 511, ...) at most 32 rows name the same one
- route_logits: bfloat16 [256, 4], P('ep'), may hold values from -8 to 300
- expert_gate: bfloat16 [128, 2048, 1024], P('ep', None, 'tp'), may hold values from -0.5 to 0.5
- expert_up: bfloat16 [128, 2048, 1024], P('ep', None, 'tp'), may hold values from -0.5 to 0.5
- expert_down: bfloat16 [128, 1024, 2048], P('ep', 'tp'), may hold values from -0.0234375 to 0.0234375
- dense_up: bfloat16 [2048, 4096], P(None, ('ep', 'tp')), may hold values from -0.125 to 0.125
- dense_down: bfloat16 [4096, 2048], P(('ep', 'tp')), may hold values from -0.09375 to 0.09375
- dense_gate: float32 [2048], replicated, may hold values from -0.125 to 0.125
Outputs:
- layer_out: bfloat16 [256, 2048], P(('ep', 'tp'))
- state_out: float32 [256, 32, 64, 128], P('ep', 'tp')
- conv_out: bfloat16 [256, 3, 2048], P('ep', None, 'tp')
- conv_proj_out: bfloat16 [256, 3, 2, 512], P('ep', None, None, 'tp')
The draws below stay inside these ranges and needn't reach their ends.
Inputs may be any that keep to these rules, and one draw needn't show every extreme that they name: `routes`: each token names 4 different experts; over the whole batch no expert is named by more than 32 rows, a bound that some block reaches.
All inputs are finite; a program needn't handle non-finite values.
Results may differ from the reference program's by a relative error of at most 0.015.
Values may be sent and summed in bfloat16 or wider, within the bound.
No kernel may reach another device: no remote copies, remote signals or barrier semaphores. Data moves between devices by JAX's collectives and lax.ppermute only.
A program may use at most 64 MiB of HBM per device.

```python
import math
import jax
import jax.numpy as jnp
import numpy as np
from jax import lax

D = 2048
HEADS = 32
HEAD_DIM = 64
STATE = 128
GROUPS = 4
KCONV = 4
DE = 1024
FD = 4096
TOPK = 4
INNER = 2048
GS = 512
EXPERTS = 128
TOKENS = 256
CAPACITY = 32


def draw_log_rate(key, part):
    return jax.random.uniform(key, (HEADS,), jnp.float32, -3.5, 1.5)


def draw_route_logits(key, part):
    base_key = jax.random.fold_in(key, 11)
    values = jnp.clip(1.5 * jax.random.normal(base_key, (TOKENS, TOPK), jnp.float32), -6.0, 6.0)
    return values.astype(jnp.bfloat16)


def steps_of(key, dims, split, low, high):
    level = 1.0
    for axis_at, parts in split:
        heights = jax.random.uniform(jax.random.fold_in(jax.random.fold_in(key, 6), axis_at), (parts,), jnp.float32, low / len(split), high / len(split))
        level = level * jnp.repeat(jnp.exp(heights), dims[axis_at] // parts).reshape((-1,) + (1,) * (len(dims) - 1 - axis_at))
    return level


def deal_out(stream_key, own, number, rows, amount, top, bound, slope):
    order = jax.random.permutation(stream_key, amount)
    packed, common = shares(amount, rows * top, bound, slope, True), shares(amount, rows * top, bound, slope, False)
    places = jnp.arange(amount)

    def named(sizes, rotation):
        used = int((sizes > 0).sum())
        fixed = max(1, used // 4)
        moved = fixed + (places - fixed + rotation * (used - fixed)) % max(1, amount - fixed)
        return jnp.zeros((amount,), jnp.int32).at[order[jnp.where(places < fixed, places, moved)]].set(jnp.asarray(sizes, jnp.int32))

    sizes = jnp.where(number % 4 == 0, named(packed, number // 4), named(common, number - number // 4 - 1))
    mixed = jax.random.permutation(jax.random.fold_in(own, 3), amount)
    giver, taker = mixed[0:amount // 2 * 2:2], mixed[1:amount // 2 * 2:2]
    room = jnp.minimum(sizes[giver] - 1, bound - sizes[taker]) // 2
    room = jnp.where((giver == order[0]) | (taker == order[0]) | (sizes[taker] == 0), 0, jnp.maximum(room, 0))
    moved = jax.random.randint(jax.random.fold_in(own, 4), (amount // 2,), 0, 1 << 20) % (room + 1)
    sizes = sizes.at[giver].add(-moved).at[taker].add(moved)
    items = jnp.searchsorted(jnp.cumsum(sizes), jnp.arange(rows * top), side="right").astype(jnp.int32)
    grid = items.reshape(top, rows).T
    grid = grid[jax.random.permutation(jax.random.fold_in(own, 1), rows)]
    rotation = jax.random.randint(jax.random.fold_in(own, 2), (rows, 1), 0, top)
    return jnp.take_along_axis(grid, (jnp.arange(top)[None, :] + rotation) % top, axis=1)


def shares(count, total, bound, skew, full):
    weights = [(1 << 20) // math.isqrt(rank ** skew) + 1 for rank in range(1, count + 1)]
    largest = bound if full else min(bound, max(-(-total // count), total * weights[0] // sum(weights)))
    least = 1 if total - largest >= count - 1 else 0
    holding, rest = [largest] + [least] * (count - 1), total - largest - least * (count - 1)
    while rest > 0:
        free = [i for i in range(1, count) if holding[i] < largest] or [i for i in range(1, count) if holding[i] < bound]
        mass, remaining = sum([weights[i] for i in free]), rest
        for i in free:
            addition = min(bound - holding[i], max(1, remaining * weights[i] // mass), rest)
            holding[i] = holding[i] + addition
            rest = rest - addition
    return np.array(holding)


def centred(key, extent, width, limit, cuts=(), kind=jnp.bfloat16):
    array = jax.random.normal(key, extent, jnp.float32) * width
    if len(cuts) > 0:
        array = steps_of(key, extent, cuts, -0.22, 0.18) * array
    return jnp.clip(array, min=-limit, max=limit).astype(kind)


def setup_inputs(seed: int = 0) -> dict:
    streams_of = jax.random.split(jax.random.key(seed), 27)
    tokens = centred(streams_of[0], (TOKENS, D), 1.0, 6.0, ((0, 128),))
    head_state = centred(streams_of[1], (TOKENS, HEADS, HEAD_DIM, STATE), 0.5, 4.0, ((0, 128), (1, 2)), jnp.float32)
    conv_state = centred(streams_of[2], (TOKENS, KCONV - 1, INNER), 1.0, 6.0, ((0, 128), (2, 2)))
    conv_proj_state = centred(streams_of[3], (TOKENS, KCONV - 1, 2, GS), 1.0, 6.0, ((0, 128), (3, 2)))
    first_gain = jnp.clip(1.0 + 0.18 * jax.random.normal(streams_of[4], (D,), jnp.float32), 0.1, 1.9)
    gate_weight = centred(streams_of[5], (D, INNER), D ** -0.5, 0.125, ((0, 128), (1, 2)))
    inner_weight = centred(streams_of[6], (D, INNER), D ** -0.5, 0.125, ((0, 128), (1, 2)))
    write_weight = centred(streams_of[7], (D, GS), D ** -0.5, 0.125, ((1, 2),))
    read_weight = centred(streams_of[8], (D, GS), D ** -0.5, 0.125, ((1, 2),))
    step_weight = centred(streams_of[9], (D, HEADS), D ** -0.5, 0.125, ((1, 2),))
    conv_kernel = centred(streams_of[10], (KCONV, INNER), 0.5, 3.0, ((1, 2),), jnp.float32)
    conv_proj_kernel = centred(streams_of[11], (KCONV, 2, GS), 0.5, 3.0, ((2, 2),), jnp.float32)
    step_bias = jnp.clip(-2.0 + 3.0 * jax.random.uniform(streams_of[12], (HEADS,), jnp.float32) ** steps_of(streams_of[12], (HEADS,), ((0, 2),), -0.2, 0.2), -2.0, 1.0)
    log_rate = draw_log_rate(jax.random.fold_in(streams_of[26], 71), 0)
    skip_gain = jnp.clip(0.5 + 1.5 * jax.random.uniform(streams_of[14], (HEADS,), jnp.float32) ** steps_of(streams_of[14], (HEADS,), ((0, 2),), -0.2, 0.2), 0.5, 2.0)
    group_gain = jnp.clip(1.0 + 0.18 * jax.random.normal(streams_of[15], (INNER,), jnp.float32), 0.1, 1.9)
    out_weight = centred(streams_of[16], (INNER, D), INNER ** -0.5, 0.125, ((0, 2), (1, 128)))
    second_gain = jnp.clip(1.0 + 0.18 * jax.random.normal(streams_of[17], (D,), jnp.float32), 0.1, 1.9)
    routes_keys = jax.random.split(jax.random.fold_in(streams_of[18], 1), TOKENS // TOKENS)
    routes_turns = jax.random.permutation(jax.random.fold_in(streams_of[18], 3), TOKENS // TOKENS)
    routes = jax.vmap(lambda own, number: deal_out(jax.random.fold_in(streams_of[18], 2), own, number, TOKENS, EXPERTS, TOPK, CAPACITY, 2))(routes_keys, routes_turns).reshape((TOKENS, TOPK))
    route_logits = draw_route_logits(jax.random.fold_in(streams_of[26], 71), 0)
    expert_gate = centred(streams_of[20], (EXPERTS, D, DE), (D // 16) ** -0.5, 0.5, ((0, 128), (2, 2)))
    expert_up = centred(streams_of[21], (EXPERTS, D, DE), (D // 16) ** -0.5, 0.5, ((0, 128), (2, 2)))
    expert_down = centred(streams_of[22], (EXPERTS, DE, D), (DE * 64) ** -0.5, 0.0234375, ((0, 128), (1, 2)))
    dense_up = centred(streams_of[23], (D, FD), D ** -0.5, 0.125, ((1, 256),))
    dense_down = centred(streams_of[24], (FD, D), FD ** -0.5, 0.09375, ((0, 256),))
    dense_gate = centred(streams_of[25], (D,), D ** -0.5, 0.125, (), jnp.float32)
    return dict(tokens=tokens, head_state=head_state, conv_state=conv_state, conv_proj_state=conv_proj_state, first_gain=first_gain, gate_weight=gate_weight, inner_weight=inner_weight, write_weight=write_weight, read_weight=read_weight, step_weight=step_weight, conv_kernel=conv_kernel, conv_proj_kernel=conv_proj_kernel, step_bias=step_bias, log_rate=log_rate, skip_gain=skip_gain, group_gain=group_gain, out_weight=out_weight, second_gain=second_gain, routes=routes, route_logits=route_logits, expert_gate=expert_gate, expert_up=expert_up, expert_down=expert_down, dense_up=dense_up, dense_down=dense_down, dense_gate=dense_gate)


norm_eps = 1e-05
clamp_limit = 7.0
glu_alpha = 1.702
highest = lax.Precision.HIGHEST

def rms_scale(values, gain_vec):
    return values * lax.rsqrt(lax.optimization_barrier(jnp.mean(values * values, axis=-1, keepdims=True)) + norm_eps) * gain_vec

def clamped_unit(gate_pre, up_pre):
    glu_part = jnp.minimum(gate_pre, clamp_limit)
    lin_part = jnp.clip(up_pre, -clamp_limit, clamp_limit)
    return glu_part * jax.nn.sigmoid(glu_alpha * glu_part) * (lin_part + 1.0)

def state_step(inner_proj, gate_proj, write_proj, read_proj, step_raw, conv_state, conv_proj_state, conv_kernel, conv_proj_kernel, step_bias, log_rate, skip_gain, group_gain, head_state, group_count):
    window_inner = jnp.concatenate([conv_state, inner_proj[:, None, :]], axis=1)
    window_proj = jnp.concatenate([conv_proj_state, jnp.stack([write_proj, read_proj], axis=1)[:, None]], axis=1)
    conv_inner = jax.nn.silu(lax.optimization_barrier(jnp.sum(window_inner.astype(jnp.float32) * conv_kernel[None], axis=1)))
    conv_proj = jax.nn.silu(lax.optimization_barrier(jnp.sum(window_proj.astype(jnp.float32) * conv_proj_kernel[None], axis=1)))
    seq_count, channels = conv_inner.shape
    head_count = step_raw.shape[1]
    head_width = channels // head_count
    state_width = conv_proj.shape[2] // group_count
    per_group = head_count // group_count
    head_input = conv_inner.reshape(seq_count, head_count, head_width)
    write_heads = jnp.repeat(conv_proj[:, 0].reshape(seq_count, group_count, state_width), per_group, axis=1)
    read_heads = jnp.repeat(conv_proj[:, 1].reshape(seq_count, group_count, state_width), per_group, axis=1)
    step_size = jax.nn.softplus(step_raw + step_bias)
    decay_rate = jnp.exp(-jnp.exp(log_rate) * step_size)
    state_out = decay_rate[:, :, None, None] * head_state + (step_size[:, :, None] * head_input)[:, :, :, None] * write_heads[:, :, None, :]
    read_out = jnp.einsum('shpn,shn->shp', state_out, read_heads, precision=highest) + skip_gain[None, :, None] * head_input
    gated_rows = read_out.reshape(seq_count, channels) * jax.nn.silu(gate_proj.astype(jnp.float32))
    grouped = gated_rows.reshape(seq_count, group_count, channels // group_count)
    grouped = grouped * lax.rsqrt(lax.optimization_barrier(jnp.mean(grouped * grouped, axis=-1, keepdims=True)) + norm_eps)
    mixer_rows = (grouped.reshape(seq_count, channels) * group_gain).astype(jnp.bfloat16)
    return (mixer_rows, state_out, window_inner[:, 1:], window_proj[:, 1:])

def reference(tokens, head_state, conv_state, conv_proj_state, first_gain, gate_weight, inner_weight, write_weight, read_weight, step_weight, conv_kernel, conv_proj_kernel, step_bias, log_rate, skip_gain, group_gain, out_weight, second_gain, routes, route_logits, expert_gate, expert_up, expert_down, dense_up, dense_down, dense_gate):
    normed_in = rms_scale(tokens.astype(jnp.float32), first_gain).astype(jnp.bfloat16)
    gate_proj = jnp.dot(normed_in, gate_weight, preferred_element_type=jnp.float32).astype(jnp.bfloat16)
    inner_proj = jnp.dot(normed_in, inner_weight, preferred_element_type=jnp.float32).astype(jnp.bfloat16)
    write_proj = jnp.dot(normed_in, write_weight, preferred_element_type=jnp.float32).astype(jnp.bfloat16)
    read_proj = jnp.dot(normed_in, read_weight, preferred_element_type=jnp.float32).astype(jnp.bfloat16)
    step_raw = jnp.dot(normed_in, step_weight, preferred_element_type=jnp.float32)
    mixer_rows, state_out, conv_out, conv_proj_out = state_step(inner_proj, gate_proj, write_proj, read_proj, step_raw, conv_state, conv_proj_state, conv_kernel, conv_proj_kernel, step_bias, log_rate, skip_gain, group_gain, head_state, GROUPS)
    mixed = jnp.dot(mixer_rows, out_weight, preferred_element_type=jnp.float32)
    hidden = (tokens.astype(jnp.float32) + mixed).astype(jnp.bfloat16)
    normed_mid = rms_scale(hidden.astype(jnp.float32), second_gain).astype(jnp.bfloat16)
    route_gates = jax.nn.softmax(route_logits.astype(jnp.float32), axis=-1)
    row_ids = jnp.arange(TOKENS, dtype=jnp.int32)

    def expert_pass(running, inputs):
        gate_block, up_block, down_block, expert_id = inputs
        route_hits = routes == expert_id
        row_weight = lax.optimization_barrier(jnp.sum(jnp.where(route_hits, route_gates, 0.0), axis=1))
        chosen = jnp.any(route_hits, axis=1)
        picked = jnp.argsort(jnp.where(chosen, row_ids, row_ids + TOKENS)).astype(jnp.int32)[:CAPACITY]
        picked_rows = normed_mid[picked]
        activated = clamped_unit(jnp.dot(picked_rows, gate_block, preferred_element_type=jnp.float32), jnp.dot(picked_rows, up_block, preferred_element_type=jnp.float32)).astype(jnp.bfloat16)
        expert_rows = jnp.dot(activated, down_block, preferred_element_type=jnp.float32) * row_weight[picked][:, None]
        return (running.at[picked].add(expert_rows), None)
    expert_ids = jnp.arange(EXPERTS, dtype=jnp.int32)
    expert_mix = lax.scan(expert_pass, jnp.zeros((TOKENS, D), jnp.float32), (expert_gate, expert_up, expert_down, expert_ids))[0]
    dense_act = jax.nn.silu(jnp.dot(normed_mid, dense_up, preferred_element_type=jnp.float32)).astype(jnp.bfloat16)
    dense_weight = jax.nn.sigmoid(jnp.dot(normed_mid.astype(jnp.float32), dense_gate, precision=highest))
    dense_value = jnp.dot(dense_act, dense_down, preferred_element_type=jnp.float32)
    layer_out = (hidden.astype(jnp.float32) + expert_mix + dense_weight[:, None] * dense_value).astype(jnp.bfloat16)
    return (layer_out, state_out, conv_out, conv_proj_out)
```

```python
import jax
import jax.numpy as jnp
from jax import lax
from jax.sharding import Mesh
from jax.sharding import PartitionSpec as P

GROUPS = 4
ROW_AXES = ("z", "y")
ROW_TP = ("z", "y", "tp")
EP = ("z", "y", "x")
EP_TP = ("z", "y", "x", "tp")


norm_eps = 1e-05
clamp_limit = 7.0
glu_alpha = 1.702
highest = lax.Precision.HIGHEST
f32 = jnp.float32
bf16 = jnp.bfloat16


def exchanged(pieces, axis):
    return lax.all_to_all(pieces, axis, split_axis=0, concat_axis=0, tiled=True)


def shifted(block, axis, by):
    size = lax.axis_size(axis)
    return lax.ppermute(block, axis, [(i, (i + by) % size) for i in range(size)])


def rms_scale(values, gain_vec):
    return (
        values * lax.rsqrt(jnp.mean(values * values, axis=-1, keepdims=True) + norm_eps) * gain_vec
    )


def clamped_unit(gate_pre, up_pre):
    glu_part = jnp.minimum(gate_pre, clamp_limit)
    lin_part = jnp.clip(up_pre, -clamp_limit, clamp_limit)
    return glu_part * jax.nn.sigmoid(glu_alpha * glu_part) * (lin_part + 1.0)


def state_step(
    inner_proj,
    gate_proj,
    write_proj,
    read_proj,
    step_raw,
    conv_state,
    conv_proj_state,
    conv_kernel,
    conv_proj_kernel,
    step_bias,
    log_rate,
    skip_gain,
    group_gain,
    head_state,
    group_count,
):
    window_inner = jnp.concatenate([conv_state, inner_proj[:, None, :]], axis=1)
    window_proj = jnp.concatenate(
        [conv_proj_state, jnp.stack([write_proj, read_proj], axis=1)[:, None]], axis=1
    )
    conv_inner = jax.nn.silu(jnp.sum(window_inner.astype(f32) * conv_kernel[None], axis=1))
    conv_proj = jax.nn.silu(jnp.sum(window_proj.astype(f32) * conv_proj_kernel[None], axis=1))
    seq_count, channels = conv_inner.shape
    head_count = step_raw.shape[1]
    head_width = channels // head_count
    state_width = conv_proj.shape[2] // group_count
    per_group = head_count // group_count
    head_input = conv_inner.reshape(seq_count, head_count, head_width)
    write_heads = jnp.repeat(
        conv_proj[:, 0].reshape(seq_count, group_count, state_width), per_group, axis=1
    )
    read_heads = jnp.repeat(
        conv_proj[:, 1].reshape(seq_count, group_count, state_width), per_group, axis=1
    )
    step_size = jax.nn.softplus(step_raw + step_bias)
    decay_rate = jnp.exp(-jnp.exp(log_rate) * step_size)
    state_out = (
        decay_rate[:, :, None, None] * head_state
        + (step_size[:, :, None] * head_input)[:, :, :, None] * write_heads[:, :, None, :]
    )
    read_out = (
        jnp.sum(state_out * read_heads[:, :, None, :], axis=-1)
        + skip_gain[None, :, None] * head_input
    )
    gated_rows = read_out.reshape(seq_count, channels) * jax.nn.silu(gate_proj.astype(f32))
    grouped = gated_rows.reshape(seq_count, group_count, channels // group_count)
    grouped = grouped * lax.rsqrt(jnp.mean(grouped * grouped, axis=-1, keepdims=True) + norm_eps)
    mixer_rows = (grouped.reshape(seq_count, channels) * group_gain).astype(bf16)
    return (mixer_rows, state_out, window_inner[:, 1:], window_proj[:, 1:])


def local(
    tokens,
    head_state,
    conv_state,
    conv_proj_state,
    first_gain,
    gate_weight,
    inner_weight,
    write_weight,
    read_weight,
    step_weight,
    conv_kernel,
    conv_proj_kernel,
    step_bias,
    log_rate,
    skip_gain,
    group_gain,
    out_weight,
    second_gain,
    routes,
    route_logits,
    expert_gate,
    expert_up,
    expert_down,
    dense_up,
    dense_down,
    dense_gate,
):
    seq_count, width = tokens.shape
    topk = routes.shape[1]
    capacity = 4 * seq_count * topk
    rows_n = lax.axis_size(ROW_AXES)
    line_n = lax.axis_size("x")
    row_at = lax.axis_index(ROW_AXES)
    line_at = lax.axis_index("x")
    tp_at = lax.axis_index("tp")
    share = gate_weight.shape[0]
    block = share * line_n
    batch = rows_n * seq_count
    channels = gate_weight.shape[1]

    normed_in = rms_scale(tokens.astype(f32), first_gain).astype(bf16)
    features = jnp.concatenate(
        [
            tokens.reshape(seq_count, rows_n, block),
            normed_in.reshape(seq_count, rows_n, block),
            jnp.broadcast_to(routes.astype(bf16)[:, None], (seq_count, rows_n, topk)),
            jnp.broadcast_to(route_logits[:, None], (seq_count, rows_n, topk)),
        ],
        axis=2,
    )
    with jax.named_scope("spread_tokens"):
        spread = exchanged(jnp.transpose(features, (1, 0, 2)), ROW_AXES)
    spread = spread.reshape(batch, 2 * block + 2 * topk)
    raw_block = spread[:, :block]
    normed_block = spread[:, block : 2 * block]
    all_routes = spread[:, 2 * block : 2 * block + topk]
    all_logits = spread[:, 2 * block + topk :].astype(f32)

    with jax.named_scope("line_weights"):
        held = jnp.concatenate(
            [
                jnp.concatenate([gate_weight, inner_weight], axis=1),
                dense_down,
                dense_up.T,
                out_weight.T.reshape(share // 2, 2 * channels),
            ],
            axis=0,
        )
        lines = jnp.stack([held] + [shifted(held, "x", -by) for by in range(1, line_n)])
    order = jnp.arange(block, dtype=jnp.int32)
    unturn = ((order[:, None] - share * line_at) % block == order[None, :]).astype(bf16)

    def natural(part):
        return jnp.dot(unturn, part, preferred_element_type=f32).astype(bf16)

    in_weight = natural(lines[:, :share].reshape(block, 2 * channels))
    line_down = lines[:, share : 2 * share].reshape(block, width)
    line_up = lines[:, 2 * share : 3 * share].reshape(block, width)
    line_out = natural(lines[:, 3 * share :].reshape(block, channels))

    with jax.named_scope("in_proj"):
        in_part = jnp.dot(normed_block, in_weight, preferred_element_type=f32).astype(bf16)
        in_terms = exchanged(in_part.reshape(rows_n, seq_count, 2 * channels), ROW_AXES)
        in_sum = jnp.sum(in_terms.astype(f32), axis=0).astype(bf16)
    gate_proj, inner_proj = in_sum[:, :channels], in_sum[:, channels:]
    write_proj = jnp.dot(normed_in, write_weight, preferred_element_type=f32).astype(bf16)
    read_proj = jnp.dot(normed_in, read_weight, preferred_element_type=f32).astype(bf16)
    step_raw = jnp.dot(normed_in, step_weight, preferred_element_type=f32)
    with jax.named_scope("state"):
        mixer_rows, state_out, conv_out, conv_proj_out = state_step(
            inner_proj,
            gate_proj,
            write_proj,
            read_proj,
            step_raw,
            conv_state,
            conv_proj_state,
            conv_kernel,
            conv_proj_kernel,
            step_bias,
            log_rate,
            skip_gain,
            group_gain,
            head_state,
            GROUPS // lax.axis_size("tp"),
        )
    with jax.named_scope("out_proj"):
        mixer_all = exchanged(
            jnp.broadcast_to(mixer_rows, (rows_n, seq_count, channels)), ROW_AXES
        ).reshape(batch, channels)
        mixed_part = lax.dot_general(
            line_out, mixer_all, (((1,), (1,)), ((), ())), preferred_element_type=f32
        )
        mixed = mixed_part + shifted(mixed_part, "tp", 1)
        hidden_block = (raw_block.T.astype(f32) + mixed).astype(bf16)
    with jax.named_scope("hidden"):
        hidden = exchanged(
            jnp.broadcast_to(hidden_block, (rows_n, block, batch)), ROW_AXES
        ).reshape(width, batch)
        hidden_wide = hidden.astype(f32)
        normed_mid = (
            hidden_wide
            * lax.rsqrt(jnp.mean(hidden_wide * hidden_wide, axis=0, keepdims=True) + norm_eps)
            * second_gain[:, None]
        ).astype(bf16)

    route_gates = jax.nn.softmax(all_logits, axis=-1)
    experts = (line_n * row_at + (line_at + jnp.arange(line_n)) % line_n).astype(bf16)
    hits = all_routes[None] == experts[:, None, None]
    row_weight = jnp.sum(jnp.where(hits, route_gates[None], 0.0), axis=2)
    chosen = jnp.any(hits, axis=2)
    earlier = (jnp.arange(batch)[:, None] < jnp.arange(batch)[None, :]).astype(bf16)
    slot = jnp.dot(chosen.astype(bf16), earlier, preferred_element_type=f32)
    slot_ids = jnp.arange(capacity, dtype=f32)
    picks = (slot[:, None, :] == slot_ids[None, :, None]) & chosen[:, None, :]
    placed = jnp.where(picks, row_weight[:, None, :], 0.0).astype(bf16)
    picks = picks.astype(bf16).reshape(line_n * capacity, batch)
    placed = placed.reshape(line_n * capacity, batch)

    with jax.named_scope("dispatch"):
        sent = lax.dot_general(
            picks, normed_mid, (((1,), (1,)), ((), ())), preferred_element_type=f32
        ).astype(bf16)
        sent = sent.reshape(line_n, capacity, width)
        rows = jnp.concatenate(
            [sent[0]] + [shifted(sent[by], "x", by) for by in range(1, line_n)], axis=0
        )
    with jax.named_scope("expert"):
        activated = clamped_unit(
            jnp.dot(rows, expert_gate[0], preferred_element_type=f32),
            jnp.dot(rows, expert_up[0], preferred_element_type=f32),
        ).astype(bf16)
        expert_rows = jnp.dot(activated, expert_down[0], preferred_element_type=f32).astype(bf16)
        expert_rows = expert_rows.reshape(line_n, capacity, width)
        returned = jnp.concatenate(
            [expert_rows[0]]
            + [shifted(expert_rows[by], "x", -by) for by in range(1, line_n)],
            axis=0,
        )
    with jax.named_scope("dense"):
        dense_weight = jax.nn.sigmoid(
            jnp.sum(normed_mid.astype(f32) * dense_gate[:, None], axis=0)
        )
        dense_inner = jax.nn.silu(
            jnp.dot(line_up, normed_mid, preferred_element_type=f32)
        ).astype(bf16)
        dense_term = (
            lax.dot_general(
                dense_inner, line_down, (((0,), (0,)), ((), ())), preferred_element_type=f32
            )
            * dense_weight[:, None]
        )
    with jax.named_scope("combine"):
        expert_term = lax.dot_general(
            placed, returned, (((0,), (0,)), ((), ())), preferred_element_type=f32
        )
        terms = (dense_term + expert_term).astype(bf16)
        terms = exchanged(terms.reshape(batch, 1, width), ROW_TP)
        own = (jnp.arange(batch) == seq_count * row_at + tp_at).astype(bf16)
        own_row = lax.dot_general(
            jnp.broadcast_to(own, (8, batch)),
            hidden,
            (((1,), (1,)), ((), ())),
            preferred_element_type=f32,
        )[:1]
        layer_out = (own_row + jnp.sum(terms.astype(f32), axis=0)).astype(bf16)
    return (layer_out, state_out, conv_out, conv_proj_out)


def solution(mesh):
    torus = Mesh(mesh.devices.reshape(8, 4, 4, mesh.shape["tp"]), EP_TP)
    return jax.shard_map(
        local,
        mesh=torus,
        in_specs=(
            P(EP, None),
            P(EP, "tp", None, None),
            P(EP, None, "tp"),
            P(EP, None, None, "tp"),
            P(),
            P(EP, "tp"),
            P(EP, "tp"),
            P(None, "tp"),
            P(None, "tp"),
            P(None, "tp"),
            P(None, "tp"),
            P(None, None, "tp"),
            P("tp"),
            P("tp"),
            P("tp"),
            P("tp"),
            P("tp", EP),
            P(),
            P(EP, None),
            P(EP, None),
            P(EP, None, "tp"),
            P(EP, None, "tp"),
            P(EP, "tp", None),
            P(None, EP_TP),
            P(EP_TP, None),
            P(),
        ),
        out_specs=(
            P(EP_TP, None),
            P(EP, "tp", None, None),
            P(EP, None, "tp"),
            P(EP, None, None, "tp"),
        ),
        check_vma=False,
    )
```

```python
import jax
import jax.numpy as jnp
from jax import lax
from jax.experimental import pallas as pl
from jax.experimental.pallas import tpu as pltpu
from jax.sharding import Mesh
from jax.sharding import PartitionSpec as P

GROUPS = 4
ROW_AXES = ("z", "y")
EP = ("z", "y", "x")
EP_TP = ("z", "y", "x", "tp")


norm_eps = 1e-05
clamp_limit = 7.0
glu_alpha = 1.702
f32 = jnp.float32
bf16 = jnp.bfloat16


def in_vmem(*arrays):
    return [pltpu.with_memory_space_constraint(a, pltpu.VMEM) for a in arrays]


def in_hbm(*arrays):
    return [pltpu.with_memory_space_constraint(a, pltpu.HBM) for a in arrays]


def exchanged(pieces, axis):
    return lax.all_to_all(pieces, axis, split_axis=0, concat_axis=0, tiled=True)


def shifted(block, axis, by):
    size = lax.axis_size(axis)
    return lax.ppermute(block, axis, [(i, (i + by) % size) for i in range(size)])


def rms_scale(values, gain_vec):
    return (
        values * lax.rsqrt(jnp.mean(values * values, axis=-1, keepdims=True) + norm_eps) * gain_vec
    )


def clamped_unit(gate_pre, up_pre):
    glu_part = jnp.minimum(gate_pre, clamp_limit)
    lin_part = jnp.clip(up_pre, -clamp_limit, clamp_limit)
    return glu_part * jax.nn.sigmoid(glu_alpha * glu_part) * (lin_part + 1.0)


def start_kernel(
    tokens,
    gain,
    routes,
    logits,
    gate_weight,
    inner_weight,
    down,
    up,
    out,
    features,
    normed_out,
    held,
    extra,
):
    seq_count, width = tokens.shape
    share, channels = gate_weight.shape
    topk = routes.shape[1]
    half = share // 2
    held[:share, :channels] = gate_weight[...]
    held[:share, channels:] = inner_weight[...]
    held[share : 2 * share, :] = down[...]
    held[2 * share : 3 * share, :] = up[...]
    held[3 * share :, :channels] = out[:half, :]
    held[3 * share :, channels:] = out[half:, :]
    raw = tokens[...].astype(f32)
    normed = rms_scale(raw, gain[...]).astype(bf16)
    normed_out[...] = normed
    normed = normed.astype(f32)
    extra[...] = jnp.zeros(extra.shape, f32)
    extra[:, :topk] = routes[...].astype(f32)
    extra[:, topk : 2 * topk] = logits[...].astype(f32)
    tail = extra[...].astype(bf16)
    first = lax.broadcasted_iota(jnp.int32, (seq_count, 128), 1) < 64
    for pair in range(width // 128):
        at = slice(128 * pair, 128 * pair + 128)
        features[2 * pair, :, :128] = jnp.where(
            first, normed[:, at], pltpu.roll(raw[:, at], 64, 1)
        ).astype(bf16)
        features[2 * pair + 1, :, :128] = jnp.where(
            first, pltpu.roll(normed[:, at], 64, 1), raw[:, at]
        ).astype(bf16)
        features[2 * pair, :, 128:] = tail
        features[2 * pair + 1, :, 128:] = tail


def in_kernel(line_at, spread, h0, h1, h2, h3, part):
    share = h0.shape[0] // 7 * 2
    block = 4 * share
    row = lax.broadcasted_iota(jnp.int32, (block, block), 0)
    column = lax.broadcasted_iota(jnp.int32, (block, block), 1)
    turn = (row == (column + share * line_at[0]) % block).astype(bf16)
    turned = jnp.dot(spread[:, :block], turn, preferred_element_type=f32).astype(bf16)
    weight = jnp.concatenate([h[:share, :] for h in (h0, h1, h2, h3)], axis=0)
    part[...] = jnp.dot(turned, weight, preferred_element_type=f32).astype(bf16)


def dispatch_kernel(picks, hidden, gain, r0, r1, r2, r3):
    rows = lax.dot_general(
        picks[...], hidden[...], (((1,), (1,)), ((), ())), preferred_element_type=f32
    )
    rows = rms_scale(rows, gain[...]).astype(bf16)
    count = r0.shape[0]
    for n, ref in enumerate((r0, r1, r2, r3)):
        ref[...] = rows[n * count : (n + 1) * count]


def dense_kernel(
    own_at,
    hidden,
    gain,
    dense_gate,
    h0,
    h1,
    h2,
    h3,
    expert_gate,
    expert_up,
    term,
    own,
    gate_near,
    up_near,
    sems,
):
    copies = (
        pltpu.make_async_copy(expert_gate.at[0], gate_near, sems.at[0]),
        pltpu.make_async_copy(expert_up.at[0], up_near, sems.at[1]),
    )
    for copy in copies:
        copy.start()
    share = h0.shape[0] // 7 * 2
    batch = hidden.shape[1]
    row = lax.broadcasted_iota(jnp.int32, (batch, batch), 0)
    column = lax.broadcasted_iota(jnp.int32, (batch, batch), 1)
    rows = lax.dot_general(
        (row == column).astype(bf16),
        hidden[...],
        (((1,), (1,)), ((), ())),
        preferred_element_type=f32,
    )
    at = lax.broadcasted_iota(jnp.int32, rows.shape, 0)
    own[...] = jnp.sum(jnp.where(at == own_at[0], rows, 0.0), axis=0, keepdims=True)
    normed = rms_scale(rows, gain[...]).astype(bf16)
    weight = jax.nn.sigmoid(
        jnp.sum(normed.astype(f32) * dense_gate[...], axis=-1, keepdims=True)
    )
    helds = (h0, h1, h2, h3)
    down = jnp.concatenate([h[share : 2 * share, :] for h in helds], axis=0)
    up = jnp.concatenate([h[2 * share : 3 * share, :] for h in helds], axis=0)
    inner = jax.nn.silu(
        lax.dot_general(normed, up, (((1,), (1,)), ((), ())), preferred_element_type=f32)
    ).astype(bf16)
    term[...] = jnp.dot(inner, down, preferred_element_type=f32) * weight
    for copy in copies:
        copy.wait()


def combine_kernel(placed, dense_term, e0, e1, e2, e3, terms):
    rows = jnp.concatenate([e0[...], e1[...], e2[...], e3[...]], axis=0)
    mix = jnp.dot(placed[...], rows, preferred_element_type=f32)
    terms[...] = (mix + dense_term[...]).astype(bf16)


def expert_kernel(own, one, two, three, gate, up, down, r0, r1, r2, r3, down_near, sems):
    _, width = down_near.shape
    parts = sems.shape[0]
    piece = width // parts
    copies = []
    for k in range(parts):
        at = pl.ds(k * piece, piece)
        copies.append(pltpu.make_async_copy(down.at[0, :, at], down_near.at[:, at], sems.at[k]))
    for copy in copies:
        copy.start()
    rows = jnp.concatenate([own[...], one[...], two[...], three[...]], axis=0)
    activated = clamped_unit(
        jnp.dot(rows, gate[...], preferred_element_type=f32),
        jnp.dot(rows, up[...], preferred_element_type=f32),
    ).astype(bf16)
    count = own.shape[0]
    for k in range(parts):
        copies[k].wait()
        at = slice(k * piece, (k + 1) * piece)
        result = jnp.dot(activated, down_near[:, at], preferred_element_type=f32).astype(bf16)
        for n, ref in enumerate((r0, r1, r2, r3)):
            ref[:, at] = result[n * count : (n + 1) * count]


def state_step(
    inner_proj,
    gate_proj,
    write_proj,
    read_proj,
    step_raw,
    conv_state,
    conv_proj_state,
    conv_kernel,
    conv_proj_kernel,
    step_bias,
    log_rate,
    skip_gain,
    group_gain,
    head_state,
    group_count,
):
    window_inner = jnp.concatenate([conv_state, inner_proj[:, None, :]], axis=1)
    window_proj = jnp.concatenate(
        [conv_proj_state, jnp.stack([write_proj, read_proj], axis=1)[:, None]], axis=1
    )
    conv_inner = jax.nn.silu(jnp.sum(window_inner.astype(f32) * conv_kernel[None], axis=1))
    conv_proj = jax.nn.silu(jnp.sum(window_proj.astype(f32) * conv_proj_kernel[None], axis=1))
    seq_count, channels = conv_inner.shape
    head_count = step_raw.shape[1]
    head_width = channels // head_count
    state_width = conv_proj.shape[2] // group_count
    per_group = head_count // group_count
    head_input = conv_inner.reshape(seq_count, head_count, head_width)
    write_heads = jnp.repeat(
        conv_proj[:, 0].reshape(seq_count, group_count, state_width), per_group, axis=1
    )
    read_heads = jnp.repeat(
        conv_proj[:, 1].reshape(seq_count, group_count, state_width), per_group, axis=1
    )
    step_size = jax.nn.softplus(step_raw + step_bias)
    decay_rate = jnp.exp(-jnp.exp(log_rate) * step_size)
    state_out = (
        decay_rate[:, :, None, None] * head_state
        + (step_size[:, :, None] * head_input)[:, :, :, None] * write_heads[:, :, None, :]
    )
    read_out = (
        jnp.sum(state_out * read_heads[:, :, None, :], axis=-1)
        + skip_gain[None, :, None] * head_input
    )
    gated_rows = read_out.reshape(seq_count, channels) * jax.nn.silu(gate_proj.astype(f32))
    grouped = gated_rows.reshape(seq_count, group_count, channels // group_count)
    grouped = grouped * lax.rsqrt(jnp.mean(grouped * grouped, axis=-1, keepdims=True) + norm_eps)
    mixer_rows = (grouped.reshape(seq_count, channels) * group_gain).astype(bf16)
    return (mixer_rows, state_out, window_inner[:, 1:], window_proj[:, 1:])


def local(
    tokens,
    head_state,
    conv_state,
    conv_proj_state,
    first_gain,
    gate_weight,
    inner_weight,
    write_weight,
    read_weight,
    step_weight,
    conv_kernel,
    conv_proj_kernel,
    step_bias,
    log_rate,
    skip_gain,
    group_gain,
    out_weight,
    second_gain,
    routes,
    route_logits,
    expert_gate,
    expert_up,
    expert_down,
    dense_up,
    dense_down,
    dense_gate,
):
    seq_count, width = tokens.shape
    topk = routes.shape[1]
    capacity = 4 * seq_count * topk
    rows_n = lax.axis_size(ROW_AXES)
    line_n = lax.axis_size("x")
    row_at = lax.axis_index(ROW_AXES)
    line_at = lax.axis_index("x")
    tp_at = lax.axis_index("tp")
    share = gate_weight.shape[0]
    block = share * line_n
    batch = rows_n * seq_count
    channels = gate_weight.shape[1]

    smem = pl.BlockSpec(memory_space=pltpu.SMEM)
    vmem = pl.BlockSpec(memory_space=pltpu.VMEM)

    lanes = 2 * block + 128
    features, normed_in, held = pl.pallas_call(
        start_kernel,
        out_shape=(
            jax.ShapeDtypeStruct((rows_n, seq_count, lanes), bf16),
            jax.ShapeDtypeStruct((seq_count, width), bf16),
            jax.ShapeDtypeStruct((3 * share + share // 2, width), bf16),
        ),
        scratch_shapes=[pltpu.VMEM((seq_count, 128), f32)],
        name="start",
            compiler_params=pltpu.CompilerParams(vmem_limit_bytes=8 << 20),
    )(
        *in_hbm(
            tokens,
            first_gain[None],
            routes,
            route_logits,
            gate_weight,
            inner_weight,
            dense_down,
            dense_up.T,
            out_weight.T,
        )
    )
    spread = exchanged(features, ROW_AXES)
    spread = spread.reshape(batch, lanes)
    raw_block = spread[:, block : 2 * block]
    all_routes = spread[:, 2 * block : 2 * block + topk]
    all_logits = spread[:, 2 * block + topk : 2 * block + 2 * topk].astype(f32)

    lines = [held] + [shifted(held, "x", -by) for by in range(1, line_n)]
    order = jnp.arange(block, dtype=jnp.int32)
    unturn = ((order[:, None] - share * line_at) % block == order[None, :]).astype(bf16)

    def natural(part):
        return jnp.dot(unturn, part, preferred_element_type=f32).astype(bf16)

    line_out = natural(
        jnp.concatenate(
            [
                part[3 * share :, at : at + channels]
                for part in lines
                for at in (0, channels)
            ],
            axis=0,
        )
    )

    in_part = pl.pallas_call(
        in_kernel,
        out_shape=pltpu.VMEM((batch, width), bf16),
        in_specs=[smem] + [vmem] * (1 + line_n),
        out_specs=vmem,
        name="in_part",
        compiler_params=pltpu.CompilerParams(vmem_limit_bytes=8 << 20),
    )(line_at.reshape(1), *in_vmem(spread, *lines))
    in_terms = exchanged(in_part.reshape(rows_n, seq_count, 2 * channels), ROW_AXES)
    in_sum = jnp.sum(in_terms.astype(f32), axis=0).astype(bf16)
    gate_proj, inner_proj = in_sum[:, :channels], in_sum[:, channels:]
    write_proj = jnp.dot(normed_in, write_weight, preferred_element_type=f32).astype(bf16)
    read_proj = jnp.dot(normed_in, read_weight, preferred_element_type=f32).astype(bf16)
    step_raw = jnp.dot(normed_in, step_weight, preferred_element_type=f32)
    mixer_rows, state_out, conv_out, conv_proj_out = state_step(
        inner_proj,
        gate_proj,
        write_proj,
        read_proj,
        step_raw,
        conv_state,
        conv_proj_state,
        conv_kernel,
        conv_proj_kernel,
        step_bias,
        log_rate,
        skip_gain,
        group_gain,
        head_state,
        GROUPS // lax.axis_size("tp"),
    )
    mixer_all = exchanged(
        jnp.broadcast_to(mixer_rows, (rows_n, seq_count, channels)), ROW_AXES
    ).reshape(batch, channels)
    mixed_part = lax.dot_general(
        line_out, mixer_all, (((1,), (1,)), ((), ())), preferred_element_type=f32
    )
    mixed = mixed_part + shifted(mixed_part, "tp", 1)
    hidden_block = (raw_block.T.astype(f32) + mixed).astype(bf16)
    hidden = exchanged(
        jnp.broadcast_to(hidden_block, (rows_n, block, batch)), ROW_AXES
    ).reshape(width, batch)

    route_gates = jax.nn.softmax(all_logits, axis=-1)
    experts = (line_n * row_at + (line_at + jnp.arange(line_n)) % line_n).astype(bf16)
    hits = all_routes[None] == experts[:, None, None]
    row_weight = jnp.sum(jnp.where(hits, route_gates[None], 0.0), axis=2)
    chosen = jnp.any(hits, axis=2)
    earlier = (jnp.arange(batch)[:, None] < jnp.arange(batch)[None, :]).astype(bf16)
    slot = jnp.dot(chosen.astype(bf16), earlier, preferred_element_type=f32)
    slot_ids = jnp.arange(capacity, dtype=f32)
    picks = (slot[:, None, :] == slot_ids[None, :, None]) & chosen[:, None, :]
    placed = jnp.where(picks, row_weight[:, None, :], 0.0).astype(bf16)
    picks = picks.astype(bf16).reshape(line_n * capacity, batch)
    placed = placed.reshape(line_n * capacity, batch).T

    sent = pl.pallas_call(
        dispatch_kernel,
        out_shape=[pltpu.VMEM((capacity, width), bf16)] * line_n,
        in_specs=[vmem] * 3,
        out_specs=[vmem] * line_n,
        name="sent",
        compiler_params=pltpu.CompilerParams(vmem_limit_bytes=8 << 20),
    )(*in_vmem(picks, hidden, second_gain[None]))
    rows = [sent[0]] + [shifted(sent[by], "x", by) for by in range(1, line_n)]
    anywhere = pl.BlockSpec(memory_space=pl.ANY)
    hidden_units = expert_gate.shape[2]
    dense_term, own_row, gate_near, up_near = pl.pallas_call(
        dense_kernel,
        out_shape=(
            pltpu.VMEM((batch, width), f32),
            pltpu.VMEM((1, width), f32),
            pltpu.VMEM((width, hidden_units), bf16),
            pltpu.VMEM((width, hidden_units), bf16),
        ),
        in_specs=[smem] + [vmem] * (3 + line_n) + [anywhere] * 2,
        out_specs=(vmem,) * 4,
        scratch_shapes=[pltpu.SemaphoreType.DMA((2,))],
        name="dense_term",
        compiler_params=pltpu.CompilerParams(vmem_limit_bytes=12 << 20),
        cost_estimate=pl.CostEstimate(
            flops=8 * batch * block * width, transcendentals=0, bytes_accessed=4 * width * 448
        ),
    )(
        (seq_count * row_at + tp_at).reshape(1),
        *in_vmem(hidden, second_gain[None], dense_gate[None], *lines),
        *in_hbm(expert_gate, expert_up),
    )
    expert_rows = pl.pallas_call(
        expert_kernel,
        out_shape=[pltpu.VMEM((capacity, width), bf16)] * line_n,
        in_specs=[vmem] * (line_n + 2) + [anywhere],
        out_specs=[vmem] * line_n,
        scratch_shapes=[
            pltpu.VMEM((hidden_units, width), bf16),
            pltpu.SemaphoreType.DMA((2,)),
        ],
        name="expert",
        compiler_params=pltpu.CompilerParams(vmem_limit_bytes=20 << 20),
    )(*in_vmem(*rows, gate_near, up_near), *in_hbm(expert_down))
    returned = [expert_rows[0]] + [shifted(expert_rows[by], "x", -by) for by in range(1, line_n)]
    terms = pl.pallas_call(
        combine_kernel,
        out_shape=pltpu.VMEM((batch, width), bf16),
        in_specs=[vmem] * (2 + line_n),
        out_specs=vmem,
        name="terms",
        compiler_params=pltpu.CompilerParams(vmem_limit_bytes=8 << 20),
    )(*in_vmem(placed, dense_term, *returned))
    terms = exchanged(terms.reshape(rows_n, seq_count, width), ROW_AXES)
    sums = jnp.sum(terms.astype(f32), axis=0)
    other = jnp.where(tp_at == 0, sums[1:], sums[:1])
    mine = jnp.where(tp_at == 0, sums[:1], sums[1:])
    layer_out = (own_row + (mine + shifted(other, "tp", 1))).astype(bf16)
    return (layer_out, state_out, conv_out, conv_proj_out)


def solution(mesh):
    torus = Mesh(mesh.devices.reshape(8, 4, 4, mesh.shape["tp"]), EP_TP)
    return jax.shard_map(
        local,
        mesh=torus,
        in_specs=(
            P(EP, None),
            P(EP, "tp", None, None),
            P(EP, None, "tp"),
            P(EP, None, None, "tp"),
            P(),
            P(EP, "tp"),
            P(EP, "tp"),
            P(None, "tp"),
            P(None, "tp"),
            P(None, "tp"),
            P(None, "tp"),
            P(None, None, "tp"),
            P("tp"),
            P("tp"),
            P("tp"),
            P("tp"),
            P("tp", EP),
            P(),
            P(EP, None),
            P(EP, None),
            P(EP, None, "tp"),
            P(EP, None, "tp"),
            P(EP, "tp", None),
            P(None, EP_TP),
            P(EP_TP, None),
            P(),
        ),
        out_specs=(
            P(EP_TP, None),
            P(EP, "tp", None, None),
            P(EP, None, "tp"),
            P(EP, None, None, "tp"),
        ),
        check_vma=False,
    )
```

```python
import jax
import jax.numpy as jnp
from jax import lax
from jax.experimental import pallas as pl
from jax.experimental.pallas import tpu as pltpu
from jax.sharding import Mesh
from jax.sharding import PartitionSpec as P

GROUPS = 4
ROW_AXES = ("z", "y")
EP = ("z", "y", "x")
EP_TP = ("z", "y", "x", "tp")


norm_eps = 1e-05
clamp_limit = 7.0
glu_alpha = 1.702
f32 = jnp.float32
bf16 = jnp.bfloat16


def in_vmem(*arrays):
    return [pltpu.with_memory_space_constraint(a, pltpu.VMEM) for a in arrays]


def in_hbm(*arrays):
    return [pltpu.with_memory_space_constraint(a, pltpu.HBM) for a in arrays]


def exchanged(pieces, axis):
    return lax.all_to_all(pieces, axis, split_axis=0, concat_axis=0, tiled=True)


def shifted(block, axis, by):
    size = lax.axis_size(axis)
    return lax.ppermute(block, axis, [(i, (i + by) % size) for i in range(size)])


def rms_scale(values, gain_vec):
    return (
        values * lax.rsqrt(jnp.mean(values * values, axis=-1, keepdims=True) + norm_eps) * gain_vec
    )


def clamped_unit(gate_pre, up_pre):
    glu_part = jnp.minimum(gate_pre, clamp_limit)
    lin_part = jnp.clip(up_pre, -clamp_limit, clamp_limit)
    return glu_part * jax.nn.sigmoid(glu_alpha * glu_part) * (lin_part + 1.0)


def start_kernel(
    tokens,
    gain,
    routes,
    logits,
    gate_weight,
    inner_weight,
    down,
    up,
    out,
    features,
    normed_out,
    held,
    extra,
):
    seq_count, width = tokens.shape
    share, channels = gate_weight.shape
    topk = routes.shape[1]
    half = share // 2
    held[:share, :channels] = gate_weight[...]
    held[:share, channels:] = inner_weight[...]
    held[share : 2 * share, :] = down[...]
    held[2 * share : 3 * share, :] = up[...]
    held[3 * share :, :channels] = out[:half, :]
    held[3 * share :, channels:] = out[half:, :]
    raw = tokens[...].astype(f32)
    normed = rms_scale(raw, gain[...]).astype(bf16)
    normed_out[...] = normed
    normed = normed.astype(f32)
    extra[...] = jnp.zeros(extra.shape, f32)
    extra[:, :topk] = routes[...].astype(f32)
    extra[:, topk : 2 * topk] = logits[...].astype(f32)
    tail = extra[...].astype(bf16)
    first = lax.broadcasted_iota(jnp.int32, (seq_count, 128), 1) < 64
    for pair in range(width // 128):
        at = slice(128 * pair, 128 * pair + 128)
        features[2 * pair, :, :128] = jnp.where(
            first, normed[:, at], pltpu.roll(raw[:, at], 64, 1)
        ).astype(bf16)
        features[2 * pair + 1, :, :128] = jnp.where(
            first, pltpu.roll(normed[:, at], 64, 1), raw[:, at]
        ).astype(bf16)
        features[2 * pair, :, 128:] = tail
        features[2 * pair + 1, :, 128:] = tail


def in_kernel(line_at, spread, h0, h1, h2, h3, part):
    share = h0.shape[0] // 7 * 2
    block = 4 * share
    row = lax.broadcasted_iota(jnp.int32, (block, block), 0)
    column = lax.broadcasted_iota(jnp.int32, (block, block), 1)
    turn = (row == (column + share * line_at[0]) % block).astype(bf16)
    turned = jnp.dot(spread[:, :block], turn, preferred_element_type=f32).astype(bf16)
    weight = jnp.concatenate([h[:share, :] for h in (h0, h1, h2, h3)], axis=0)
    part[...] = jnp.dot(turned, weight, preferred_element_type=f32).astype(bf16)


def out_kernel(line_at, mixer, h0, h1, h2, h3, part):
    share = h0.shape[0] // 7 * 2
    block, channels = part.shape[0], mixer.shape[1]
    row = lax.broadcasted_iota(jnp.int32, (block, block), 0)
    column = lax.broadcasted_iota(jnp.int32, (block, block), 1)
    turn = (column == (row + block - share * line_at[0]) % block).astype(bf16)
    weight = jnp.concatenate(
        [
            h[3 * share :, at : at + channels].astype(f32)
            for h in (h0, h1, h2, h3)
            for at in (0, channels)
        ],
        axis=0,
    ).astype(bf16)
    weight = jnp.dot(turn, weight, preferred_element_type=f32).astype(bf16)
    part[...] = lax.dot_general(
        weight, mixer[...], (((1,), (1,)), ((), ())), preferred_element_type=f32
    )


def hidden_kernel(part, other, spread, pieces):
    block, _ = part.shape
    row = lax.broadcasted_iota(jnp.int32, (block, 2 * block), 0)
    column = lax.broadcasted_iota(jnp.int32, (block, 2 * block), 1)
    raw = lax.dot_general(
        (column == row + block).astype(bf16),
        spread[:, : 2 * block],
        (((1,), (1,)), ((), ())),
        preferred_element_type=f32,
    )
    hidden = raw + (part[...] + other[...])
    half = block // 2
    packed = jnp.concatenate([hidden[:half], hidden[half:]], axis=1).astype(bf16)
    pieces[...] = jnp.broadcast_to(packed[None], pieces.shape)


def unpacked(pieces):
    count, half, lanes = pieces.shape
    low = pieces[...]
    flat = low.reshape(count * half, lanes).astype(f32)
    high = pltpu.roll(flat, lanes // 2, 1).astype(bf16).reshape(count, half, lanes)
    return jnp.concatenate([low, high], axis=1).reshape(2 * count * half, lanes)


def dispatch_kernel(picks, pieces, gain, r0, r1, r2, r3):
    rows = lax.dot_general(
        picks[...], unpacked(pieces), (((1,), (1,)), ((), ())), preferred_element_type=f32
    )
    rows = rms_scale(rows, gain[...]).astype(bf16)
    count = r0.shape[0]
    for n, ref in enumerate((r0, r1, r2, r3)):
        ref[...] = rows[n * count : (n + 1) * count]


def dense_kernel(
    own_at,
    pieces,
    gain,
    dense_gate,
    h0,
    h1,
    h2,
    h3,
    expert_gate,
    expert_up,
    term,
    own,
    gate_near,
    up_near,
    sems,
):
    copies = (
        pltpu.make_async_copy(expert_gate.at[0], gate_near, sems.at[0]),
        pltpu.make_async_copy(expert_up.at[0], up_near, sems.at[1]),
    )
    for copy in copies:
        copy.start()
    share = h0.shape[0] // 7 * 2
    batch = term.shape[0]
    row = lax.broadcasted_iota(jnp.int32, (batch, 2 * batch), 0)
    column = lax.broadcasted_iota(jnp.int32, (batch, 2 * batch), 1)
    rows = lax.dot_general(
        (row == column).astype(bf16),
        unpacked(pieces),
        (((1,), (1,)), ((), ())),
        preferred_element_type=f32,
    )
    at = lax.broadcasted_iota(jnp.int32, rows.shape, 0)
    own[...] = jnp.sum(jnp.where(at == own_at[0], rows, 0.0), axis=0, keepdims=True)
    normed = rms_scale(rows, gain[...]).astype(bf16)
    weight = jax.nn.sigmoid(
        jnp.sum(normed.astype(f32) * dense_gate[...], axis=-1, keepdims=True)
    )
    helds = (h0, h1, h2, h3)
    down = jnp.concatenate([h[share : 2 * share, :] for h in helds], axis=0)
    up = jnp.concatenate([h[2 * share : 3 * share, :] for h in helds], axis=0)
    inner = jax.nn.silu(
        lax.dot_general(normed, up, (((1,), (1,)), ((), ())), preferred_element_type=f32)
    ).astype(bf16)
    term[...] = jnp.dot(inner, down, preferred_element_type=f32) * weight
    for copy in copies:
        copy.wait()


def combine_kernel(placed, dense_term, e0, e1, e2, e3, terms):
    rows = jnp.concatenate([e0[...], e1[...], e2[...], e3[...]], axis=0)
    mix = jnp.dot(placed[...], rows, preferred_element_type=f32)
    terms[...] = (mix + dense_term[...]).astype(bf16)


def expert_kernel(own, one, two, three, gate, up, down, r0, r1, r2, r3, down_near, sems):
    _, width = down_near.shape
    parts = sems.shape[0]
    piece = width // parts
    copies = []
    for k in range(parts):
        at = pl.ds(k * piece, piece)
        copies.append(pltpu.make_async_copy(down.at[0, :, at], down_near.at[:, at], sems.at[k]))
    for copy in copies:
        copy.start()
    rows = jnp.concatenate([own[...], one[...], two[...], three[...]], axis=0)
    activated = clamped_unit(
        jnp.dot(rows, gate[...], preferred_element_type=f32),
        jnp.dot(rows, up[...], preferred_element_type=f32),
    ).astype(bf16)
    count = own.shape[0]
    for k in range(parts):
        copies[k].wait()
        at = slice(k * piece, (k + 1) * piece)
        result = jnp.dot(activated, down_near[:, at], preferred_element_type=f32).astype(bf16)
        for n, ref in enumerate((r0, r1, r2, r3)):
            ref[:, at] = result[n * count : (n + 1) * count]


def state_step(
    inner_proj,
    gate_proj,
    write_proj,
    read_proj,
    step_raw,
    conv_state,
    conv_proj_state,
    conv_kernel,
    conv_proj_kernel,
    step_bias,
    log_rate,
    skip_gain,
    group_gain,
    head_state,
    group_count,
):
    window_inner = jnp.concatenate([conv_state, inner_proj[:, None, :]], axis=1)
    window_proj = jnp.concatenate(
        [conv_proj_state, jnp.stack([write_proj, read_proj], axis=1)[:, None]], axis=1
    )
    conv_inner = jax.nn.silu(jnp.sum(window_inner.astype(f32) * conv_kernel[None], axis=1))
    conv_proj = jax.nn.silu(jnp.sum(window_proj.astype(f32) * conv_proj_kernel[None], axis=1))
    seq_count, channels = conv_inner.shape
    head_count = step_raw.shape[1]
    head_width = channels // head_count
    state_width = conv_proj.shape[2] // group_count
    per_group = head_count // group_count
    head_input = conv_inner.reshape(seq_count, head_count, head_width)
    write_heads = jnp.repeat(
        conv_proj[:, 0].reshape(seq_count, group_count, state_width), per_group, axis=1
    )
    read_heads = jnp.repeat(
        conv_proj[:, 1].reshape(seq_count, group_count, state_width), per_group, axis=1
    )
    step_size = jax.nn.softplus(step_raw + step_bias)
    decay_rate = jnp.exp(-jnp.exp(log_rate) * step_size)
    old_read = jnp.sum(head_state * read_heads[:, :, None, :], axis=-1) * decay_rate[:, :, None]
    direct = step_size * jnp.sum(write_heads * read_heads, axis=-1) + skip_gain
    read_out = old_read + direct[:, :, None] * head_input
    gated_rows = read_out.reshape(seq_count, channels) * jax.nn.silu(gate_proj.astype(f32))
    grouped = gated_rows.reshape(seq_count, group_count, channels // group_count)
    grouped = grouped * lax.rsqrt(jnp.mean(grouped * grouped, axis=-1, keepdims=True) + norm_eps)
    mixer_rows = (grouped.reshape(seq_count, channels) * group_gain).astype(bf16)
    mixer_rows, head_state = lax.optimization_barrier((mixer_rows, head_state))
    state_out = (
        decay_rate[:, :, None, None] * head_state
        + (step_size[:, :, None] * head_input)[:, :, :, None] * write_heads[:, :, None, :]
    )
    return (mixer_rows, state_out, window_inner[:, 1:], window_proj[:, 1:])


def local(
    tokens,
    head_state,
    conv_state,
    conv_proj_state,
    first_gain,
    gate_weight,
    inner_weight,
    write_weight,
    read_weight,
    step_weight,
    conv_kernel,
    conv_proj_kernel,
    step_bias,
    log_rate,
    skip_gain,
    group_gain,
    out_weight,
    second_gain,
    routes,
    route_logits,
    expert_gate,
    expert_up,
    expert_down,
    dense_up,
    dense_down,
    dense_gate,
):
    seq_count, width = tokens.shape
    topk = routes.shape[1]
    capacity = 4 * seq_count * topk
    rows_n = lax.axis_size(ROW_AXES)
    line_n = lax.axis_size("x")
    row_at = lax.axis_index(ROW_AXES)
    line_at = lax.axis_index("x")
    tp_at = lax.axis_index("tp")
    share = gate_weight.shape[0]
    block = share * line_n
    batch = rows_n * seq_count
    channels = gate_weight.shape[1]

    smem = pl.BlockSpec(memory_space=pltpu.SMEM)
    vmem = pl.BlockSpec(memory_space=pltpu.VMEM)

    lanes = 2 * block + 128
    features, normed_in, held = pl.pallas_call(
        start_kernel,
        out_shape=(
            jax.ShapeDtypeStruct((rows_n, seq_count, lanes), bf16),
            jax.ShapeDtypeStruct((seq_count, width), bf16),
            jax.ShapeDtypeStruct((3 * share + share // 2, width), bf16),
        ),
        scratch_shapes=[pltpu.VMEM((seq_count, 128), f32)],
        name="start",
            compiler_params=pltpu.CompilerParams(vmem_limit_bytes=8 << 20),
    )(
        *in_hbm(
            tokens,
            first_gain[None],
            routes,
            route_logits,
            gate_weight,
            inner_weight,
            dense_down,
            dense_up.T,
            out_weight.T,
        )
    )
    spread = exchanged(features, ROW_AXES)
    spread = spread.reshape(batch, lanes)
    all_routes = spread[:, 2 * block : 2 * block + topk]
    all_logits = spread[:, 2 * block + topk : 2 * block + 2 * topk].astype(f32)

    lines = [held] + [shifted(held, "x", -by) for by in range(1, line_n)]
    in_part = pl.pallas_call(
        in_kernel,
        out_shape=pltpu.VMEM((batch, width), bf16),
        in_specs=[smem] + [vmem] * (1 + line_n),
        out_specs=vmem,
        name="in_part",
        compiler_params=pltpu.CompilerParams(vmem_limit_bytes=8 << 20),
    )(line_at.reshape(1), *in_vmem(spread, *lines))
    in_terms = exchanged(in_part.reshape(rows_n, seq_count, 2 * channels), ROW_AXES)
    in_sum = jnp.sum(in_terms.astype(f32), axis=0).astype(bf16)
    gate_proj, inner_proj = in_sum[:, :channels], in_sum[:, channels:]
    write_proj = jnp.dot(normed_in, write_weight, preferred_element_type=f32).astype(bf16)
    read_proj = jnp.dot(normed_in, read_weight, preferred_element_type=f32).astype(bf16)
    step_raw = jnp.dot(normed_in, step_weight, preferred_element_type=f32)
    mixer_rows, state_out, conv_out, conv_proj_out = state_step(
        inner_proj,
        gate_proj,
        write_proj,
        read_proj,
        step_raw,
        conv_state,
        conv_proj_state,
        conv_kernel,
        conv_proj_kernel,
        step_bias,
        log_rate,
        skip_gain,
        group_gain,
        head_state,
        GROUPS // lax.axis_size("tp"),
    )
    mixer_all = exchanged(
        jnp.broadcast_to(mixer_rows, (rows_n, seq_count, channels)), ROW_AXES
    ).reshape(batch, channels)
    mixed_part = pl.pallas_call(
        out_kernel,
        out_shape=pltpu.VMEM((block, batch), f32),
        in_specs=[smem] + [vmem] * (1 + line_n),
        out_specs=vmem,
        name="out_part",
        compiler_params=pltpu.CompilerParams(vmem_limit_bytes=8 << 20),
    )(line_at.reshape(1), *in_vmem(mixer_all, *lines))
    other_part = shifted(mixed_part, "tp", 1)
    pieces = pl.pallas_call(
        hidden_kernel,
        out_shape=jax.ShapeDtypeStruct((rows_n, block // 2, 2 * batch), bf16),
        in_specs=[vmem] * 3,
        out_specs=vmem,
        name="hidden_pieces",
        compiler_params=pltpu.CompilerParams(vmem_limit_bytes=8 << 20),
    )(*in_vmem(mixed_part, other_part, spread))
    hidden = exchanged(pieces, ROW_AXES)

    route_gates = jax.nn.softmax(all_logits, axis=-1)
    experts = (line_n * row_at + (line_at + jnp.arange(line_n)) % line_n).astype(bf16)
    hits = all_routes[None] == experts[:, None, None]
    row_weight = jnp.sum(jnp.where(hits, route_gates[None], 0.0), axis=2)
    chosen = jnp.any(hits, axis=2)
    earlier = (jnp.arange(batch)[:, None] < jnp.arange(batch)[None, :]).astype(bf16)
    slot = jnp.dot(chosen.astype(bf16), earlier, preferred_element_type=f32)
    slot_ids = jnp.arange(capacity, dtype=f32)
    picks = (slot[:, None, :] == slot_ids[None, :, None]) & chosen[:, None, :]
    placed = jnp.where(picks, row_weight[:, None, :], 0.0).astype(bf16)
    picks = jnp.pad(
        picks.astype(bf16).reshape(line_n * capacity, batch), ((0, 0), (0, batch))
    )
    placed = placed.reshape(line_n * capacity, batch).T

    sent = pl.pallas_call(
        dispatch_kernel,
        out_shape=[pltpu.VMEM((capacity, width), bf16)] * line_n,
        in_specs=[vmem] * 3,
        out_specs=[vmem] * line_n,
        name="sent",
        compiler_params=pltpu.CompilerParams(vmem_limit_bytes=8 << 20),
    )(*in_vmem(picks, hidden, second_gain[None]))
    rows = [sent[0]] + [shifted(sent[by], "x", by) for by in range(1, line_n)]
    anywhere = pl.BlockSpec(memory_space=pl.ANY)
    hidden_units = expert_gate.shape[2]
    dense_term, own_row, gate_near, up_near = pl.pallas_call(
        dense_kernel,
        out_shape=(
            pltpu.VMEM((batch, width), f32),
            pltpu.VMEM((1, width), f32),
            pltpu.VMEM((width, hidden_units), bf16),
            pltpu.VMEM((width, hidden_units), bf16),
        ),
        in_specs=[smem] + [vmem] * (3 + line_n) + [anywhere] * 2,
        out_specs=(vmem,) * 4,
        scratch_shapes=[pltpu.SemaphoreType.DMA((2,))],
        name="dense_term",
        compiler_params=pltpu.CompilerParams(vmem_limit_bytes=12 << 20),
        cost_estimate=pl.CostEstimate(
            flops=8 * batch * block * width, transcendentals=0, bytes_accessed=4 * width * 448
        ),
    )(
        (seq_count * row_at + tp_at).reshape(1),
        *in_vmem(hidden, second_gain[None], dense_gate[None], *lines),
        *in_hbm(expert_gate, expert_up),
    )
    expert_rows = pl.pallas_call(
        expert_kernel,
        out_shape=[pltpu.VMEM((capacity, width), bf16)] * line_n,
        in_specs=[vmem] * (line_n + 2) + [anywhere],
        out_specs=[vmem] * line_n,
        scratch_shapes=[
            pltpu.VMEM((hidden_units, width), bf16),
            pltpu.SemaphoreType.DMA((2,)),
        ],
        name="expert",
        compiler_params=pltpu.CompilerParams(vmem_limit_bytes=20 << 20),
    )(*in_vmem(*rows, gate_near, up_near), *in_hbm(expert_down))
    returned = [expert_rows[0]] + [shifted(expert_rows[by], "x", -by) for by in range(1, line_n)]
    terms = pl.pallas_call(
        combine_kernel,
        out_shape=pltpu.VMEM((batch, width), bf16),
        in_specs=[vmem] * (2 + line_n),
        out_specs=vmem,
        name="terms",
        compiler_params=pltpu.CompilerParams(vmem_limit_bytes=8 << 20),
    )(*in_vmem(placed, dense_term, *returned))
    terms = exchanged(terms.reshape(rows_n, seq_count, width), ROW_AXES)
    sums = jnp.sum(terms.astype(f32), axis=0)
    other = jnp.where(tp_at == 0, sums[1:], sums[:1])
    mine = jnp.where(tp_at == 0, sums[:1], sums[1:])
    layer_out = (own_row + (mine + shifted(other, "tp", 1))).astype(bf16)
    return (layer_out, state_out, conv_out, conv_proj_out)


def solution(mesh):
    torus = Mesh(mesh.devices.reshape(8, 4, 4, mesh.shape["tp"]), EP_TP)
    return jax.shard_map(
        local,
        mesh=torus,
        in_specs=(
            P(EP, None),
            P(EP, "tp", None, None),
            P(EP, None, "tp"),
            P(EP, None, None, "tp"),
            P(),
            P(EP, "tp"),
            P(EP, "tp"),
            P(None, "tp"),
            P(None, "tp"),
            P(None, "tp"),
            P(None, "tp"),
            P(None, None, "tp"),
            P("tp"),
            P("tp"),
            P("tp"),
            P("tp"),
            P("tp", EP),
            P(),
            P(EP, None),
            P(EP, None),
            P(EP, None, "tp"),
            P(EP, None, "tp"),
            P(EP, "tp", None),
            P(None, EP_TP),
            P(EP_TP, None),
            P(),
        ),
        out_specs=(
            P(EP_TP, None),
            P(EP, "tp", None, None),
            P(EP, None, "tp"),
            P(EP, None, None, "tp"),
        ),
        check_vma=False,
    )
```

```python
import jax
import jax.numpy as jnp
from jax import lax
from jax.experimental import pallas as pl
from jax.experimental.pallas import tpu as pltpu
from jax.sharding import Mesh
from jax.sharding import PartitionSpec as P

GROUPS = 4
ROW_AXES = ("z", "y")
EP = ("z", "y", "x")
EP_TP = ("z", "y", "x", "tp")


norm_eps = 1e-05
clamp_limit = 7.0
glu_alpha = 1.702
f32 = jnp.float32
bf16 = jnp.bfloat16


def in_vmem(*arrays):
    return [pltpu.with_memory_space_constraint(a, pltpu.VMEM) for a in arrays]


def in_hbm(*arrays):
    return [pltpu.with_memory_space_constraint(a, pltpu.HBM) for a in arrays]


def exchanged(pieces, axis):
    return lax.all_to_all(pieces, axis, split_axis=0, concat_axis=0, tiled=True)


def shifted(block, axis, by):
    size = lax.axis_size(axis)
    return lax.ppermute(block, axis, [(i, (i + by) % size) for i in range(size)])


def rms_scale(values, gain_vec):
    return (
        values * lax.rsqrt(jnp.mean(values * values, axis=-1, keepdims=True) + norm_eps) * gain_vec
    )


def clamped_unit(gate_pre, up_pre):
    glu_part = jnp.minimum(gate_pre, clamp_limit)
    lin_part = jnp.clip(up_pre, -clamp_limit, clamp_limit)
    return glu_part * jax.nn.sigmoid(glu_alpha * glu_part) * (lin_part + 1.0)


def start_kernel(
    tokens,
    gain,
    routes,
    logits,
    gate_weight,
    inner_weight,
    down,
    up,
    out,
    features,
    normed_out,
    held,
    extra,
):
    seq_count, width = tokens.shape
    share, channels = gate_weight.shape
    topk = routes.shape[1]
    half = share // 2
    held[:share, :channels] = gate_weight[...]
    held[:share, channels:] = inner_weight[...]
    held[share : 2 * share, :] = down[...]
    held[2 * share : 3 * share, :] = up[...]
    held[3 * share :, :channels] = out[:half, :]
    held[3 * share :, channels:] = out[half:, :]
    raw = tokens[...].astype(f32)
    normed = rms_scale(raw, gain[...]).astype(bf16)
    normed_out[...] = normed
    normed = normed.astype(f32)
    extra[...] = jnp.zeros(extra.shape, f32)
    extra[:, :topk] = routes[...].astype(f32)
    extra[:, topk : 2 * topk] = logits[...].astype(f32)
    tail = extra[...].astype(bf16)
    first = lax.broadcasted_iota(jnp.int32, (seq_count, 128), 1) < 64
    for pair in range(width // 128):
        at = slice(128 * pair, 128 * pair + 128)
        features[2 * pair, :, :128] = jnp.where(
            first, normed[:, at], pltpu.roll(raw[:, at], 64, 1)
        ).astype(bf16)
        features[2 * pair + 1, :, :128] = jnp.where(
            first, pltpu.roll(normed[:, at], 64, 1), raw[:, at]
        ).astype(bf16)
        features[2 * pair, :, 128:] = tail
        features[2 * pair + 1, :, 128:] = tail


def in_kernel(line_at, spread, h0, h1, h2, h3, part):
    share = h0.shape[0] // 7 * 2
    block = 4 * share
    row = lax.broadcasted_iota(jnp.int32, (block, block), 0)
    column = lax.broadcasted_iota(jnp.int32, (block, block), 1)
    turn = (row == (column + share * line_at[0]) % block).astype(bf16)
    turned = jnp.dot(spread[:, :block], turn, preferred_element_type=f32).astype(bf16)
    weight = jnp.concatenate([h[:share, :] for h in (h0, h1, h2, h3)], axis=0)
    result = jnp.dot(turned, weight, preferred_element_type=f32).astype(bf16)
    part[...] = result.reshape(part.shape)


def out_kernel(line_at, mixer, h0, h1, h2, h3, part):
    share = h0.shape[0] // 7 * 2
    block, channels = part.shape[0], mixer.shape[1]
    row = lax.broadcasted_iota(jnp.int32, (block, block), 0)
    column = lax.broadcasted_iota(jnp.int32, (block, block), 1)
    turn = (column == (row + block - share * line_at[0]) % block).astype(bf16)
    weight = jnp.concatenate(
        [
            h[3 * share :, at : at + channels].astype(f32)
            for h in (h0, h1, h2, h3)
            for at in (0, channels)
        ],
        axis=0,
    ).astype(bf16)
    weight = jnp.dot(turn, weight, preferred_element_type=f32).astype(bf16)
    part[...] = lax.dot_general(
        weight, mixer[...], (((1,), (1,)), ((), ())), preferred_element_type=f32
    )


def hidden_kernel(part, other, spread, pieces):
    block, _ = part.shape
    row = lax.broadcasted_iota(jnp.int32, (block, 2 * block), 0)
    column = lax.broadcasted_iota(jnp.int32, (block, 2 * block), 1)
    raw = lax.dot_general(
        (column == row + block).astype(bf16),
        spread[:, : 2 * block],
        (((1,), (1,)), ((), ())),
        preferred_element_type=f32,
    )
    hidden = raw + (part[...] + other[...])
    half = block // 2
    packed = jnp.concatenate([hidden[:half], hidden[half:]], axis=1).astype(bf16)
    pieces[...] = jnp.broadcast_to(packed[None], pieces.shape)


def unpacked(pieces):
    count, half, lanes = pieces.shape
    low = pieces[...]
    flat = low.reshape(count * half, lanes).astype(f32)
    high = pltpu.roll(flat, lanes // 2, 1).astype(bf16).reshape(count, half, lanes)
    return jnp.concatenate([low, high], axis=1).reshape(2 * count * half, lanes)


def dispatch_kernel(picks, pieces, gain, r0, r1, r2, r3):
    rows = lax.dot_general(
        picks[...], unpacked(pieces), (((1,), (1,)), ((), ())), preferred_element_type=f32
    )
    rows = rms_scale(rows, gain[...]).astype(bf16)
    count = r0.shape[0]
    for n, ref in enumerate((r0, r1, r2, r3)):
        ref[...] = rows[n * count : (n + 1) * count]


def dense_kernel(
    own_at,
    pieces,
    gain,
    dense_gate,
    h0,
    h1,
    h2,
    h3,
    expert_gate,
    expert_up,
    term,
    own,
    gate_near,
    up_near,
    sems,
):
    copies = (
        pltpu.make_async_copy(expert_gate.at[0], gate_near, sems.at[0]),
        pltpu.make_async_copy(expert_up.at[0], up_near, sems.at[1]),
    )
    for copy in copies:
        copy.start()
    share = h0.shape[0] // 7 * 2
    batch = term.shape[0]
    row = lax.broadcasted_iota(jnp.int32, (batch, 2 * batch), 0)
    column = lax.broadcasted_iota(jnp.int32, (batch, 2 * batch), 1)
    rows = lax.dot_general(
        (row == column).astype(bf16),
        unpacked(pieces),
        (((1,), (1,)), ((), ())),
        preferred_element_type=f32,
    )
    at = lax.broadcasted_iota(jnp.int32, rows.shape, 0)
    own[...] = jnp.sum(jnp.where(at == own_at[0], rows, 0.0), axis=0, keepdims=True)
    normed = rms_scale(rows, gain[...]).astype(bf16)
    weight = jax.nn.sigmoid(
        jnp.sum(normed.astype(f32) * dense_gate[...], axis=-1, keepdims=True)
    )
    helds = (h0, h1, h2, h3)
    down = jnp.concatenate([h[share : 2 * share, :] for h in helds], axis=0)
    up = jnp.concatenate([h[2 * share : 3 * share, :] for h in helds], axis=0)
    inner = jax.nn.silu(
        lax.dot_general(normed, up, (((1,), (1,)), ((), ())), preferred_element_type=f32)
    ).astype(bf16)
    term[...] = jnp.dot(inner, down, preferred_element_type=f32) * weight
    for copy in copies:
        copy.wait()


def combine_kernel(placed, dense_term, e0, e1, e2, e3, terms):
    rows = jnp.concatenate([e0[...], e1[...], e2[...], e3[...]], axis=0)
    mix = jnp.dot(placed[...], rows, preferred_element_type=f32)
    terms[...] = (mix + dense_term[...]).astype(bf16).reshape(terms.shape)


def expert_kernel(own, one, two, three, gate, up, down, r0, r1, r2, r3, down_near, sems):
    _, width = down_near.shape
    parts = sems.shape[0]
    piece = width // parts
    copies = []
    for k in range(parts):
        at = pl.ds(k * piece, piece)
        copies.append(pltpu.make_async_copy(down.at[0, :, at], down_near.at[:, at], sems.at[k]))
    for copy in copies:
        copy.start()
    rows = jnp.concatenate([own[...], one[...], two[...], three[...]], axis=0)
    activated = clamped_unit(
        jnp.dot(rows, gate[...], preferred_element_type=f32),
        jnp.dot(rows, up[...], preferred_element_type=f32),
    ).astype(bf16)
    count = own.shape[0]
    for k in range(parts):
        copies[k].wait()
        at = slice(k * piece, (k + 1) * piece)
        result = jnp.dot(activated, down_near[:, at], preferred_element_type=f32).astype(bf16)
        for n, ref in enumerate((r0, r1, r2, r3)):
            ref[:, at] = result[n * count : (n + 1) * count]


def state_step(
    inner_proj,
    gate_proj,
    write_proj,
    read_proj,
    step_raw,
    conv_state,
    conv_proj_state,
    conv_kernel,
    conv_proj_kernel,
    step_bias,
    log_rate,
    skip_gain,
    group_gain,
    head_state,
    group_count,
):
    window_inner = jnp.concatenate([conv_state, inner_proj[:, None, :]], axis=1)
    window_proj = jnp.concatenate(
        [conv_proj_state, jnp.stack([write_proj, read_proj], axis=1)[:, None]], axis=1
    )
    conv_inner = jax.nn.silu(jnp.sum(window_inner.astype(f32) * conv_kernel[None], axis=1))
    conv_proj = jax.nn.silu(jnp.sum(window_proj.astype(f32) * conv_proj_kernel[None], axis=1))
    seq_count, channels = conv_inner.shape
    head_count = step_raw.shape[1]
    head_width = channels // head_count
    state_width = conv_proj.shape[2] // group_count
    per_group = head_count // group_count
    head_input = conv_inner.reshape(seq_count, head_count, head_width)
    write_heads = jnp.repeat(
        conv_proj[:, 0].reshape(seq_count, group_count, state_width), per_group, axis=1
    )
    read_heads = jnp.repeat(
        conv_proj[:, 1].reshape(seq_count, group_count, state_width), per_group, axis=1
    )
    step_size = jax.nn.softplus(step_raw + step_bias)
    decay_rate = jnp.exp(-jnp.exp(log_rate) * step_size)
    old_read = jnp.sum(head_state * read_heads[:, :, None, :], axis=-1) * decay_rate[:, :, None]
    direct = step_size * jnp.sum(write_heads * read_heads, axis=-1) + skip_gain
    read_out = old_read + direct[:, :, None] * head_input
    gated_rows = read_out.reshape(seq_count, channels) * jax.nn.silu(gate_proj.astype(f32))
    grouped = gated_rows.reshape(seq_count, group_count, channels // group_count)
    grouped = grouped * lax.rsqrt(jnp.mean(grouped * grouped, axis=-1, keepdims=True) + norm_eps)
    mixer_rows = (grouped.reshape(seq_count, channels) * group_gain).astype(bf16)
    mixer_rows, head_state = lax.optimization_barrier((mixer_rows, head_state))
    state_out = (
        decay_rate[:, :, None, None] * head_state
        + (step_size[:, :, None] * head_input)[:, :, :, None] * write_heads[:, :, None, :]
    )
    return (mixer_rows, state_out, window_inner[:, 1:], window_proj[:, 1:])


def local(
    tokens,
    head_state,
    conv_state,
    conv_proj_state,
    first_gain,
    gate_weight,
    inner_weight,
    write_weight,
    read_weight,
    step_weight,
    conv_kernel,
    conv_proj_kernel,
    step_bias,
    log_rate,
    skip_gain,
    group_gain,
    out_weight,
    second_gain,
    routes,
    route_logits,
    expert_gate,
    expert_up,
    expert_down,
    dense_up,
    dense_down,
    dense_gate,
):
    seq_count, width = tokens.shape
    topk = routes.shape[1]
    capacity = 4 * seq_count * topk
    rows_n = lax.axis_size(ROW_AXES)
    line_n = lax.axis_size("x")
    row_at = lax.axis_index(ROW_AXES)
    line_at = lax.axis_index("x")
    tp_at = lax.axis_index("tp")
    share = gate_weight.shape[0]
    block = share * line_n
    batch = rows_n * seq_count
    channels = gate_weight.shape[1]

    smem = pl.BlockSpec(memory_space=pltpu.SMEM)
    vmem = pl.BlockSpec(memory_space=pltpu.VMEM)

    lanes = 2 * block + 128
    features, normed_in, held = pl.pallas_call(
        start_kernel,
        out_shape=(
            jax.ShapeDtypeStruct((rows_n, seq_count, lanes), bf16),
            jax.ShapeDtypeStruct((seq_count, width), bf16),
            jax.ShapeDtypeStruct((3 * share + share // 2, width), bf16),
        ),
        scratch_shapes=[pltpu.VMEM((seq_count, 128), f32)],
        name="start",
            compiler_params=pltpu.CompilerParams(vmem_limit_bytes=8 << 20),
    )(
        *in_hbm(
            tokens,
            first_gain[None],
            routes,
            route_logits,
            gate_weight,
            inner_weight,
            dense_down,
            dense_up.T,
            out_weight.T,
        )
    )
    spread = exchanged(features, ROW_AXES)
    spread = spread.reshape(batch, lanes)

    lines = [held] + [shifted(held, "x", -by) for by in range(1, line_n)]
    in_part = pl.pallas_call(
        in_kernel,
        out_shape=jax.ShapeDtypeStruct((rows_n, seq_count, width), bf16),
        in_specs=[smem] + [vmem] * (1 + line_n),
        out_specs=vmem,
        name="in_part",
        compiler_params=pltpu.CompilerParams(vmem_limit_bytes=8 << 20),
    )(line_at.reshape(1), *in_vmem(spread, *lines))
    in_terms = exchanged(in_part, ROW_AXES)
    in_sum = jnp.sum(in_terms.astype(f32), axis=0).astype(bf16)
    gate_proj, inner_proj = in_sum[:, :channels], in_sum[:, channels:]
    write_proj = jnp.dot(normed_in, write_weight, preferred_element_type=f32).astype(bf16)
    read_proj = jnp.dot(normed_in, read_weight, preferred_element_type=f32).astype(bf16)
    step_raw = jnp.dot(normed_in, step_weight, preferred_element_type=f32)
    mixer_rows, state_out, conv_out, conv_proj_out = state_step(
        inner_proj,
        gate_proj,
        write_proj,
        read_proj,
        step_raw,
        conv_state,
        conv_proj_state,
        conv_kernel,
        conv_proj_kernel,
        step_bias,
        log_rate,
        skip_gain,
        group_gain,
        head_state,
        GROUPS // lax.axis_size("tp"),
    )
    mixer_all = exchanged(
        jnp.broadcast_to(mixer_rows, (rows_n, seq_count, channels)), ROW_AXES
    ).reshape(batch, channels)
    mixed_part = pl.pallas_call(
        out_kernel,
        out_shape=pltpu.VMEM((block, batch), f32),
        in_specs=[smem] + [vmem] * (1 + line_n),
        out_specs=vmem,
        name="out_part",
        compiler_params=pltpu.CompilerParams(vmem_limit_bytes=8 << 20),
    )(line_at.reshape(1), *in_vmem(mixer_all, *lines))
    other_part = shifted(mixed_part, "tp", 1)
    pieces = pl.pallas_call(
        hidden_kernel,
        out_shape=jax.ShapeDtypeStruct((rows_n, block // 2, 2 * batch), bf16),
        in_specs=[vmem] * 3,
        out_specs=vmem,
        name="hidden_pieces",
        compiler_params=pltpu.CompilerParams(vmem_limit_bytes=8 << 20),
    )(*in_vmem(mixed_part, other_part, spread))
    hidden = exchanged(pieces, ROW_AXES)

    all_routes = spread[:, 2 * block : 2 * block + topk]
    all_logits = spread[:, 2 * block + topk : 2 * block + 2 * topk].astype(f32)
    route_gates = jax.nn.softmax(all_logits, axis=-1)
    experts = (line_n * row_at + (line_at + jnp.arange(line_n)) % line_n).astype(bf16)
    hits = all_routes[None] == experts[:, None, None]
    row_weight = jnp.sum(jnp.where(hits, route_gates[None], 0.0), axis=2)
    chosen = jnp.any(hits, axis=2)
    earlier = (jnp.arange(batch)[:, None] < jnp.arange(batch)[None, :]).astype(bf16)
    slot = jnp.dot(chosen.astype(bf16), earlier, preferred_element_type=f32)
    slot_ids = jnp.arange(capacity, dtype=f32)
    picks = (slot[:, None, :] == slot_ids[None, :, None]) & chosen[:, None, :]
    placed = jnp.where(picks, row_weight[:, None, :], 0.0).astype(bf16)
    picks = jnp.pad(
        picks.astype(bf16).reshape(line_n * capacity, batch), ((0, 0), (0, batch))
    )
    placed = placed.reshape(line_n * capacity, batch).T

    sent = pl.pallas_call(
        dispatch_kernel,
        out_shape=[pltpu.VMEM((capacity, width), bf16)] * line_n,
        in_specs=[vmem] * 3,
        out_specs=[vmem] * line_n,
        name="sent",
        compiler_params=pltpu.CompilerParams(vmem_limit_bytes=8 << 20),
    )(*in_vmem(picks, hidden, second_gain[None]))
    rows = [sent[0]] + [shifted(sent[by], "x", by) for by in range(1, line_n)]
    anywhere = pl.BlockSpec(memory_space=pl.ANY)
    hidden_units = expert_gate.shape[2]
    dense_term, own_row, gate_near, up_near = pl.pallas_call(
        dense_kernel,
        out_shape=(
            pltpu.VMEM((batch, width), f32),
            pltpu.VMEM((1, width), f32),
            pltpu.VMEM((width, hidden_units), bf16),
            pltpu.VMEM((width, hidden_units), bf16),
        ),
        in_specs=[smem] + [vmem] * (3 + line_n) + [anywhere] * 2,
        out_specs=(vmem,) * 4,
        scratch_shapes=[pltpu.SemaphoreType.DMA((2,))],
        name="dense_term",
        compiler_params=pltpu.CompilerParams(vmem_limit_bytes=12 << 20),
        cost_estimate=pl.CostEstimate(
            flops=8 * batch * block * width, transcendentals=0, bytes_accessed=4 * width * 448
        ),
    )(
        (seq_count * row_at + tp_at).reshape(1),
        *in_vmem(hidden, second_gain[None], dense_gate[None], *lines),
        *in_hbm(expert_gate, expert_up),
    )
    expert_rows = pl.pallas_call(
        expert_kernel,
        out_shape=[pltpu.VMEM((capacity, width), bf16)] * line_n,
        in_specs=[vmem] * (line_n + 2) + [anywhere],
        out_specs=[vmem] * line_n,
        scratch_shapes=[
            pltpu.VMEM((hidden_units, width), bf16),
            pltpu.SemaphoreType.DMA((2,)),
        ],
        name="expert",
        compiler_params=pltpu.CompilerParams(vmem_limit_bytes=20 << 20),
    )(*in_vmem(*rows, gate_near, up_near), *in_hbm(expert_down))
    returned = [expert_rows[0]] + [shifted(expert_rows[by], "x", -by) for by in range(1, line_n)]
    terms = pl.pallas_call(
        combine_kernel,
        out_shape=jax.ShapeDtypeStruct((rows_n, seq_count, width), bf16),
        in_specs=[vmem] * (2 + line_n),
        out_specs=vmem,
        name="terms",
        compiler_params=pltpu.CompilerParams(vmem_limit_bytes=8 << 20),
    )(*in_vmem(placed, dense_term, *returned))
    terms = exchanged(terms, ROW_AXES)
    sums = jnp.sum(terms.astype(f32), axis=0)
    other = jnp.where(tp_at == 0, sums[1:], sums[:1])
    mine = jnp.where(tp_at == 0, sums[:1], sums[1:])
    layer_out = (own_row + (mine + shifted(other, "tp", 1))).astype(bf16)
    return (layer_out, state_out, conv_out, conv_proj_out)


def solution(mesh):
    torus = Mesh(mesh.devices.reshape(8, 4, 4, mesh.shape["tp"]), EP_TP)
    return jax.shard_map(
        local,
        mesh=torus,
        in_specs=(
            P(EP, None),
            P(EP, "tp", None, None),
            P(EP, None, "tp"),
            P(EP, None, None, "tp"),
            P(),
            P(EP, "tp"),
            P(EP, "tp"),
            P(None, "tp"),
            P(None, "tp"),
            P(None, "tp"),
            P(None, "tp"),
            P(None, None, "tp"),
            P("tp"),
            P("tp"),
            P("tp"),
            P("tp"),
            P("tp", EP),
            P(),
            P(EP, None),
            P(EP, None),
            P(EP, None, "tp"),
            P(EP, None, "tp"),
            P(EP, "tp", None),
            P(None, EP_TP),
            P(EP_TP, None),
            P(),
        ),
        out_specs=(
            P(EP_TP, None),
            P(EP, "tp", None, None),
            P(EP, None, "tp"),
            P(EP, None, None, "tp"),
        ),
        check_vma=False,
    )
```
